32 devices in a mesh: kv: 16 (over z, y, x), tp: 2 (over core).
Axes of the slice: x: 2, y: 2, z: 4, core: 2. Of those that a mesh axis runs over, the one named last changes fastest.
Arguments:
- tokens: bfloat16 [6144, 2048], P('kv', 'tp'), may hold values from -12 to 12
- query_weight: bfloat16 [2048, 2048], P(None, 'tp'), may hold values from -0.5 to 0.5
- key_weight: bfloat16 [2048, 1024], P(None, 'tp'), may hold values from -0.5 to 0.5
- value_weight: bfloat16 [2048, 1024], P(None, 'tp'), may hold values from -0.125 to 0.125
- out_weight: bfloat16 [2048, 2048], P(None, 'tp'), may hold values from -0.125 to 0.125
- chosen: int32 [96, 16], P('kv'), may hold values from 0 to 95, as said below
Outputs:
- mixed: bfloat16 [6144, 2048], P('kv', 'tp')
The draws below stay inside these ranges and needn't reach their ends.
Inputs may be any that keep to these rules, and one draw needn't show every extreme that they name: `chosen`: row b names no block after b; its first entry is b and its next 3 entries are blocks of the same device as block b; entries may repeat. Over the rows of one device, the entries after the first 4 name at most 2 blocks, counting repeats, of any one other device, and some device names exactly 2 of another.
All inputs are finite; a program needn't handle non-finite values.
Results may differ from the reference program's by a relative error of at most 0.0072.
Values may be sent and summed in bfloat16 or wider, within the bound.
A program may use at most 128 MiB of HBM per device.

```python
import jax
import jax.numpy as jnp
from jax import lax

D = 2048
H = 16
KVH = 8
HD = 128
BLK = 64
TOPB = 16
LOCAL = 3
CAP = 2
TOK_DEV = 384
TOKENS = 6144
NQB = 96
N_KV = 16


def draw_tokens(key, part):
    plain = jnp.clip(jax.random.normal(key, (TOKENS, D), jnp.float32), -6.0, 6.0)
    return plain.astype(jnp.bfloat16)


def draw_query_weight(key, part):
    fresh = jax.random.normal(jax.random.fold_in(key, 11), (D, H * HD), jnp.float32)
    return jnp.clip(fresh * D ** (-0.5), -0.5, 0.5).astype(jnp.bfloat16)


def draw_key_weight(key, part):
    fresh = jax.random.normal(jax.random.fold_in(key, 12), (D, KVH * HD), jnp.float32)
    return jnp.clip(fresh * D ** (-0.5), -0.5, 0.5).astype(jnp.bfloat16)


def draw_chosen(key, part):
    blocks = TOK_DEV // BLK
    far_count = TOPB - 1 - LOCAL
    ask_count = blocks * far_count
    picked = min(ask_count // CAP, N_KV)
    streams = jax.random.split(jax.random.fold_in(key, 21), 6)
    devices = jnp.arange(N_KV, dtype=jnp.int32)
    asking = devices[:, None]
    target = devices[None, :]
    raw_score = jax.random.randint(streams[0], (N_KV, N_KV), 0, 1 << 14)
    popular = jax.random.randint(streams[1], (1, N_KV), 0, 4) == 0
    forced = (target == asking - 1) | (target == asking - N_KV // 2)
    scores = raw_score * 1024 + target
    scores = scores + jnp.where(popular, 1 << 25, 0) + jnp.where(forced, 1 << 26, 0)
    scores = jnp.where(target < asking, scores, -1 - target)
    ranked = lax.top_k(scores, picked)[1].astype(jnp.int32)
    usable = jnp.minimum(devices, picked)
    request = jnp.arange(ask_count, dtype=jnp.int32)
    owner_slot = request // CAP
    holder = jnp.take_along_axis(ranked, jnp.broadcast_to(jnp.minimum(owner_slot, picked - 1)[None, :], (N_KV, ask_count)), axis=1)
    usable_slot = owner_slot[None, :] < usable[:, None]
    hot_block = jax.random.randint(streams[2], (N_KV,), 0, blocks)
    coin_flip = jax.random.randint(streams[3], (N_KV, ask_count), 0, 2)
    any_block = jax.random.randint(streams[4], (N_KV, ask_count), 0, blocks)
    inside = jnp.where(coin_flip == 0, hot_block[holder], any_block)
    query_block = devices[:, None] * blocks + request[None, :] // far_count
    far_ids = jnp.where(usable_slot, holder * blocks + inside, query_block).reshape(N_KV, blocks, far_count)
    own_ids = devices[:, None] * blocks + jnp.arange(blocks, dtype=jnp.int32)[None, :]
    near_raw = jax.random.randint(streams[5], (N_KV, blocks, LOCAL), 0, 1 << 16)
    near_ids = devices[:, None, None] * blocks + near_raw % (jnp.arange(blocks, dtype=jnp.int32)[None, :, None] + 1)
    table_rows = jnp.concatenate([own_ids[:, :, None], near_ids, far_ids], axis=2)
    return table_rows.reshape(N_KV * blocks, TOPB).astype(jnp.int32)


def steps_of(rng, extent, cuts, low, largest):
    loudness = 1.0
    for axis_at, blocks in cuts:
        steps = jax.random.uniform(jax.random.fold_in(jax.random.fold_in(rng, 6), axis_at), (blocks,), jnp.float32, low / len(cuts), largest / len(cuts))
        loudness = loudness * jnp.repeat(jnp.exp(steps), extent[axis_at] // blocks).reshape((-1,) + (1,) * (len(extent) - 1 - axis_at))
    return loudness


def centred(rng, dims, width, limit, cuts=(), kind=jnp.bfloat16):
    values = jax.random.normal(rng, dims, jnp.float32) * width
    if len(cuts) > 0:
        values = steps_of(rng, dims, cuts, -0.22, 0.18) * values
    return jnp.clip(values, min=-limit, max=limit).astype(kind)


def setup_inputs(seed: int = 0) -> dict:
    keys = jax.random.split(jax.random.key(seed), 7)
    return {
        "tokens": draw_tokens(jax.random.fold_in(keys[6], 71), 0),
        "query_weight": draw_query_weight(jax.random.fold_in(keys[6], 71), 0),
        "key_weight": draw_key_weight(jax.random.fold_in(keys[6], 71), 0),
        "value_weight": centred(keys[3], (D, KVH * HD), D ** -0.5, 0.125, ((1, 2),)),
        "out_weight": centred(keys[4], (H * HD, D), (H * HD) ** -0.5, 0.125, ((1, 2),)),
        "chosen": draw_chosen(jax.random.fold_in(keys[6], 71), 0),
    }


def reference(tokens, query_weight, key_weight, value_weight, out_weight, chosen):
    queries = jnp.dot(tokens, query_weight, preferred_element_type=jnp.float32).astype(jnp.bfloat16)
    key_rows = jnp.dot(tokens, key_weight, preferred_element_type=jnp.float32).astype(jnp.bfloat16)
    value_rows = jnp.dot(tokens, value_weight, preferred_element_type=jnp.float32).astype(jnp.bfloat16)
    group_size = H // KVH
    grouped = queries.reshape(NQB, BLK, KVH, group_size, HD)
    key_blocks = key_rows.reshape(NQB, BLK, KVH, HD)
    value_blocks = value_rows.reshape(NQB, BLK, KVH, HD)

    def attend(inputs):
        block_queries, chosen_row, block_number = inputs
        slot_order = jnp.arange(TOPB)
        repeats = jnp.any((chosen_row[:, None] == chosen_row[None, :]) & (slot_order[None, :] < slot_order[:, None]), axis=1)
        got_keys = jnp.take(key_blocks, chosen_row, axis=0).reshape(TOPB * BLK, KVH, HD)
        got_values = jnp.take(value_blocks, chosen_row, axis=0).reshape(TOPB * BLK, KVH, HD)
        scores = jnp.einsum("qkgd,skd->kgqs", block_queries.astype(jnp.float32), got_keys.astype(jnp.float32),
                            precision=lax.Precision.HIGHEST) * (HD ** -0.5)
        query_pos = block_number * BLK + jnp.arange(BLK, dtype=jnp.int32)
        key_pos = (chosen_row[:, None] * BLK + jnp.arange(BLK, dtype=jnp.int32)[None, :]).reshape(-1)
        fresh_slot = jnp.broadcast_to((~repeats)[:, None], (TOPB, BLK)).reshape(-1)
        visible = fresh_slot[None, :] & (key_pos[None, :] <= query_pos[:, None])
        scores = jnp.where(visible[None, None], scores, -jnp.inf)
        row_peak = jnp.max(scores, axis=-1, keepdims=True)
        weights = jnp.exp(scores - row_peak)
        row_total = jnp.sum(weights, axis=-1)
        rounded = lax.optimization_barrier(weights.astype(jnp.bfloat16)).astype(jnp.float32)
        mixed_heads = jnp.einsum("kgqs,skd->qkgd", rounded, got_values.astype(jnp.float32),
                                 precision=lax.Precision.HIGHEST)
        mixed_heads = mixed_heads / jnp.transpose(row_total, (2, 0, 1))[..., None]
        return mixed_heads.astype(jnp.bfloat16).reshape(BLK, H * HD)

    heads_out = lax.map(attend, (grouped, chosen, jnp.arange(NQB, dtype=jnp.int32)))
    return jnp.dot(heads_out.reshape(TOKENS, H * HD), out_weight, preferred_element_type=jnp.float32).astype(jnp.bfloat16)
```

```python
import functools
import math

import jax
import jax.numpy as jnp
from jax import lax
from jax.experimental import pallas as pl
from jax.experimental.pallas import tpu as pltpu
from jax.sharding import PartitionSpec as P

HD = 128
BLK = 64
TOPB = 16
CAP = 2
PLANE = 4
VMEM = pltpu.MemorySpace.VMEM
SMEM = pltpu.MemorySpace.SMEM


def select_kernel(peers, index_ref, shard_ref, *out_refs):
    for peer in range(peers):
        for place in range(CAP):
            row = pl.multiple_of(index_ref[peer * CAP + place] * BLK, BLK)
            out_refs[peer][place * BLK:(place + 1) * BLK, :] = shard_ref[pl.ds(row, BLK), :]


def select(index, shard, peers):
    cols = shard.shape[1]
    shape = jax.ShapeDtypeStruct((CAP * BLK, cols), shard.dtype)
    return pl.pallas_call(
        functools.partial(select_kernel, peers),
        out_shape=[shape] * peers,
        in_specs=[pl.BlockSpec(memory_space=SMEM), pl.BlockSpec(memory_space=VMEM)],
        out_specs=[pl.BlockSpec(memory_space=VMEM)] * peers,
        cost_estimate=pl.CostEstimate(flops=0, bytes_accessed=4 * peers * CAP * BLK * cols, transcendentals=0),
    )(index, shard)


def attend_kernel(key_heads, group, count, rows_ref, q_ref, bias_ref, *refs):
    sources = refs[:count]
    out_ref, held, picked, sems = refs[count:]
    key_cols = key_heads * HD
    own_blocks = q_ref.shape[0] // BLK
    copies = []
    start = 0
    for at, source in enumerate(sources):
        size = source.shape[0]
        copies.append(pltpu.make_async_copy(source, held.at[start:start + size], sems.at[at]))
        start += size
    for copy in copies:
        copy.start()
    for copy in copies:
        copy.wait()
    wide = (group * BLK, TOPB * BLK)
    row_at = lax.broadcasted_iota(jnp.int32, wide, 0) % BLK
    col_at = lax.broadcasted_iota(jnp.int32, wide, 1)
    later = (col_at < BLK) & (col_at > row_at)

    def one(b, _):
        for slot in range(TOPB):
            row = pl.multiple_of(rows_ref[b * TOPB + slot] * BLK, BLK)
            picked[slot * BLK:(slot + 1) * BLK, :] = held[pl.ds(row, BLK), :]
        first = pl.multiple_of(b * BLK, BLK)
        bias = bias_ref[b]
        for head in range(key_heads):
            q = jnp.concatenate(
                [q_ref[pl.ds(first, BLK), (head * group + g) * HD:(head * group + g + 1) * HD] for g in range(group)],
                axis=0,
            )
            keys = picked[:, head * HD:(head + 1) * HD]
            values = picked[:, key_cols + head * HD:key_cols + (head + 1) * HD]
            scores = lax.dot_general(
                q, keys, (((1,), (1,)), ((), ())), preferred_element_type=jnp.float32
            ) * HD ** (-0.5)
            scores = jnp.where(later, -jnp.inf, scores + bias)
            peak = jnp.max(scores, axis=1, keepdims=True)
            weights = jnp.exp(scores - peak)
            total = jnp.sum(weights, axis=1, keepdims=True)
            mixed = jnp.dot(weights.astype(jnp.bfloat16), values, preferred_element_type=jnp.float32) / total
            mixed = mixed.astype(jnp.bfloat16)
            for g in range(group):
                at = (head * group + g) * HD
                out_ref[pl.ds(first, BLK), at:at + HD] = mixed[g * BLK:(g + 1) * BLK]
        return 0

    lax.fori_loop(0, own_blocks, one, 0)


def attend(rows, queries, bias, sources):
    tok_rows, query_cols = queries.shape
    key_cols = sources[0].shape[1] // 2
    key_heads = key_cols // HD
    group = query_cols // key_cols
    count = len(sources)
    held_rows = sum(s.shape[0] for s in sources)
    pairs = tok_rows * TOPB * BLK * (query_cols // HD)
    return pl.pallas_call(
        functools.partial(attend_kernel, key_heads, group, count),
        out_shape=jax.ShapeDtypeStruct((tok_rows, query_cols), jnp.bfloat16),
        in_specs=[pl.BlockSpec(memory_space=SMEM), pl.BlockSpec(memory_space=VMEM), pl.BlockSpec(memory_space=VMEM)]
        + [pl.BlockSpec(memory_space=pl.ANY)] * count,
        out_specs=pl.BlockSpec(memory_space=VMEM),
        scratch_shapes=[
            pltpu.VMEM((held_rows, 2 * key_cols), jnp.bfloat16),
            pltpu.VMEM((TOPB * BLK, 2 * key_cols), jnp.bfloat16),
            pltpu.SemaphoreType.DMA((count,)),
        ],
        compiler_params=pltpu.CompilerParams(vmem_limit_bytes=32 * 2**20),
        cost_estimate=pl.CostEstimate(
            flops=4 * pairs * HD, bytes_accessed=4 * held_rows * key_cols, transcendentals=pairs
        ),
    )(rows, queries, bias, *sources)


def turned(x, shift):
    size = lax.axis_size("tp")
    return lax.ppermute(x, "tp", [((i + shift) % size, i) for i in range(size)])


def shares(x):
    size = lax.axis_size("tp")
    me = lax.axis_index("tp")
    return [(x if s == 0 else turned(x, s), (me + s) % size) for s in range(size)]


def project(parts, weight):
    depth = parts[0][0].shape[1]
    total = None
    for block, owner in parts:
        rows = lax.dynamic_slice_in_dim(weight, owner * depth, depth, axis=0)
        term = jnp.dot(block, rows, preferred_element_type=jnp.float32)
        total = term if total is None else total + term
    return total.astype(jnp.bfloat16)


def local(tokens, query_weight, key_weight, value_weight, out_weight, chosen):
    tok_rows = tokens.shape[0]
    own_blocks = tok_rows // BLK
    key_devices = lax.axis_size("kv")
    plane = math.gcd(key_devices, PLANE)
    layers = key_devices // plane
    device = lax.axis_index("kv")
    my_layer, my_seat = device // plane, device % plane

    wanted = chosen.reshape(-1)
    holder = wanted // own_blocks
    within = wanted % own_blocks
    remote = holder != device
    slot_index = jnp.arange(wanted.shape[0])
    earlier = (
        (slot_index[None, :] < slot_index[:, None])
        & (holder[None, :] == holder[:, None])
        & remote[None, :]
    )
    places = jnp.minimum(jnp.sum(earlier.astype(jnp.int32), axis=1), CAP - 1)
    back = my_layer - holder // plane
    across = (holder % plane) ^ my_seat
    hop = (back * plane + across) * CAP + places
    asked = jnp.arange(layers * plane * CAP)
    request = jnp.sum(
        jnp.where((hop[None, :] == asked[:, None]) & remote[None, :], within[None, :], 0), axis=1
    ).reshape(layers, plane, CAP)
    asks = [
        lax.ppermute(request[:, m], "kv", [(i, i ^ m) for i in range(key_devices)])
        for m in range(1, plane)
    ]

    parts = shares(tokens)
    column = jnp.concatenate([project(parts, key_weight), project(parts, value_weight)], axis=1)
    upward = [(i, i + plane) for i in range(key_devices - plane)]
    columns, arrived = [], []
    for k in range(layers):
        columns.append(column)
        if k + 1 < layers:
            onward = lax.ppermute(column, "kv", upward)
        if plane > 1:
            index = jnp.concatenate([ask[k] for ask in asks])
            for m, block in enumerate(select(index, column, plane - 1), 1):
                arrived.append(lax.ppermute(block, "kv", [(i, i ^ m) for i in range(key_devices)]))
        column = onward
    queries = project(parts, query_weight)

    near_rows = back * own_blocks + within
    far_rows = layers * own_blocks + (back * (plane - 1) + across - 1) * CAP + places
    rows = jnp.where(across == 0, near_rows, far_rows).astype(jnp.int32)
    order = jnp.arange(TOPB)
    repeats = jnp.any(
        (chosen[:, :, None] == chosen[:, None, :]) & (order[None, None, :] < order[None, :, None]), axis=2
    )
    bias = jnp.repeat(jnp.where(repeats, -jnp.inf, 0.0).astype(jnp.float32), BLK, axis=1)
    heads_out = attend(rows, queries, bias[:, None, :], columns + arrived)
    return project(shares(heads_out), out_weight)


def solution(mesh):
    return jax.shard_map(
        local,
        mesh=mesh,
        in_specs=(
            P("kv", "tp"),
            P(None, "tp"),
            P(None, "tp"),
            P(None, "tp"),
            P(None, "tp"),
            P("kv", None),
        ),
        out_specs=P("kv", "tp"),
        check_vma=False,
    )
```

```python
import functools
import math

import jax
import jax.numpy as jnp
from jax import lax
from jax.experimental import pallas as pl
from jax.experimental.pallas import tpu as pltpu
from jax.sharding import PartitionSpec as P

HD = 128
BLK = 64
TOPB = 16
CAP = 2
PLANE = 4
VMEM = pltpu.MemorySpace.VMEM
SMEM = pltpu.MemorySpace.SMEM


def exchange_kernel(plane, layers, k_ref, v_ref, ask_ref, heldk, heldv, stage, asked, asked_s,
                    up_send, up_recv, side_send, side_recv, ask_send, ask_recv, move_sem):
    me = lax.axis_index("kv")
    core = lax.axis_index("tp")
    layer = me // plane
    seat = me % plane
    tok_rows = k_ref.shape[0]
    own = (k_ref, v_ref)
    held = (heldk, heldv)
    peers = [layer * plane + (seat ^ m) for m in range(1, plane)]
    above = layer + 1 < layers
    below = layer > 0

    def at(device):
        return {"device_id": (device, core), "device_id_type": pl.DeviceIdType.MESH}

    barrier = pltpu.get_barrier_semaphore()
    for peer in peers:
        pl.semaphore_signal(barrier, inc=1, **at(peer))

    @pl.when(above)
    def _():
        pl.semaphore_signal(barrier, inc=1, **at(me + plane))

    @pl.when(below)
    def _():
        pl.semaphore_signal(barrier, inc=1, **at(me - plane))

    between = above & below

    @pl.when(between)
    def _():
        pl.semaphore_wait(barrier, plane + 1)

    @pl.when(jnp.logical_not(between))
    def _():
        pl.semaphore_wait(barrier, plane - 1 + min(layers - 1, 1))

    def climb(k, half):
        source = own[half] if k == 0 else held[half].at[k * tok_rows:(k + 1) * tok_rows]
        return pltpu.make_async_remote_copy(
            src_ref=source,
            dst_ref=held[half].at[(k + 1) * tok_rows:(k + 2) * tok_rows],
            send_sem=up_send.at[k, half],
            recv_sem=up_recv.at[k, half],
            **at(me + plane),
        )

    def side(k, half, m):
        first = layers * tok_rows + (k * (plane - 1) + m) * CAP * BLK
        return pltpu.make_async_remote_copy(
            src_ref=stage.at[k, half, m],
            dst_ref=held[half].at[first:first + CAP * BLK],
            send_sem=side_send.at[k, half, m],
            recv_sem=side_recv.at[k, half, m],
            **at(peers[m]),
        )

    def tell(m):
        return pltpu.make_async_remote_copy(
            src_ref=ask_ref.at[m], dst_ref=asked.at[m], send_sem=ask_send.at[m], recv_sem=ask_recv.at[m],
            **at(peers[m]),
        )

    for half in range(2):
        @pl.when(above)
        def _():
            climb(0, half).start()
    for m in range(plane - 1):
        tell(m).start()
    for half in range(2):
        held[half][0:tok_rows, :] = own[half][...]
    for m in range(plane - 1):
        tell(m).wait()
    move = pltpu.make_async_copy(asked, asked_s, move_sem)
    move.start()
    move.wait()

    for k in range(layers):
        for half in range(2):
            @pl.when(layer >= k)
            def _():
                if k > 0:
                    climb(k - 1, half).wait_recv()
                    if k + 1 < layers:
                        @pl.when(above)
                        def _():
                            climb(k, half).start()
                for m in range(plane - 1):
                    for place in range(CAP):
                        block = asked_s[m, 0, k * CAP + place]
                        taken = held[half][k * tok_rows:k * tok_rows + BLK, :]
                        for other in range(1, tok_rows // BLK):
                            first = k * tok_rows + other * BLK
                            taken = jnp.where(block == other, held[half][first:first + BLK, :], taken)
                        stage[k, half, m, place * BLK:(place + 1) * BLK, :] = taken
                    side(k, half, m).start()

    for k in range(layers):
        @pl.when(layer >= k)
        def _():
            for half in range(2):
                for m in range(plane - 1):
                    side(k, half, m).wait()
        if k + 1 < layers:
            @pl.when(above & (layer >= k))
            def _():
                for half in range(2):
                    climb(k, half).wait_send()


def exchange(keys, values, ask, plane, layers):
    tok_rows, cols = keys.shape
    held_rows = layers * (tok_rows + (plane - 1) * CAP * BLK)
    shape = jax.ShapeDtypeStruct((held_rows, cols), keys.dtype)
    peers = plane - 1
    dma = pltpu.SemaphoreType.DMA
    return pl.pallas_call(
        functools.partial(exchange_kernel, plane, layers),
        out_shape=[shape] * 2,
        in_specs=[pl.BlockSpec(memory_space=VMEM)] * 3,
        out_specs=[pl.BlockSpec(memory_space=VMEM)] * 2,
        scratch_shapes=[
            pltpu.VMEM((layers, 2, peers, CAP * BLK, cols), keys.dtype),
            pltpu.VMEM(ask.shape, ask.dtype),
            pltpu.SMEM(ask.shape, ask.dtype),
            dma((layers, 2)), dma((layers, 2)),
            dma((layers, 2, peers)), dma((layers, 2, peers)),
            dma((peers,)), dma((peers,)), dma(()),
        ],
        compiler_params=pltpu.CompilerParams(
            collective_id=0, has_side_effects=True, vmem_limit_bytes=40 * 2**20
        ),
    )(keys, values, ask)


def attend_kernel(key_heads, group, rows_ref, q_ref, bias_ref, heldk, heldv, out_ref, pickk, pickv):
    own_blocks = q_ref.shape[0] // BLK
    wide = (group * BLK, TOPB * BLK)
    row_at = lax.broadcasted_iota(jnp.int32, wide, 0) % BLK
    col_at = lax.broadcasted_iota(jnp.int32, wide, 1)
    later = (col_at < BLK) & (col_at > row_at)

    def one(b, _):
        for slot in range(TOPB):
            row = pl.multiple_of(rows_ref[b * TOPB + slot] * BLK, BLK)
            pickk[slot * BLK:(slot + 1) * BLK, :] = heldk[pl.ds(row, BLK), :]
            pickv[slot * BLK:(slot + 1) * BLK, :] = heldv[pl.ds(row, BLK), :]
        first = pl.multiple_of(b * BLK, BLK)
        bias = bias_ref[b]
        for head in range(key_heads):
            q = jnp.concatenate(
                [q_ref[pl.ds(first, BLK), (head * group + g) * HD:(head * group + g + 1) * HD] for g in range(group)],
                axis=0,
            )
            keys = pickk[:, head * HD:(head + 1) * HD]
            values = pickv[:, head * HD:(head + 1) * HD]
            scores = lax.dot_general(
                q, keys, (((1,), (1,)), ((), ())), preferred_element_type=jnp.float32
            ) * HD ** (-0.5)
            scores = jnp.where(later, -jnp.inf, scores + bias)
            peak = jnp.max(scores, axis=1, keepdims=True)
            weights = jnp.exp(scores - peak)
            total = jnp.sum(weights, axis=1, keepdims=True)
            mixed = jnp.dot(weights.astype(jnp.bfloat16), values, preferred_element_type=jnp.float32) / total
            mixed = mixed.astype(jnp.bfloat16)
            for g in range(group):
                at = (head * group + g) * HD
                out_ref[pl.ds(first, BLK), at:at + HD] = mixed[g * BLK:(g + 1) * BLK]
        return 0

    lax.fori_loop(0, own_blocks, one, 0)


def attend(rows, queries, bias, heldk, heldv):
    tok_rows, query_cols = queries.shape
    held_rows, key_cols = heldk.shape
    key_heads = key_cols // HD
    group = query_cols // key_cols
    pairs = tok_rows * TOPB * BLK * (query_cols // HD)
    return pl.pallas_call(
        functools.partial(attend_kernel, key_heads, group),
        out_shape=jax.ShapeDtypeStruct((tok_rows, query_cols), jnp.bfloat16),
        in_specs=[pl.BlockSpec(memory_space=SMEM)] + [pl.BlockSpec(memory_space=VMEM)] * 4,
        out_specs=pl.BlockSpec(memory_space=VMEM),
        scratch_shapes=[pltpu.VMEM((TOPB * BLK, key_cols), jnp.bfloat16)] * 2,
        compiler_params=pltpu.CompilerParams(vmem_limit_bytes=32 * 2**20),
        cost_estimate=pl.CostEstimate(
            flops=4 * pairs * HD, bytes_accessed=4 * held_rows * key_cols, transcendentals=pairs
        ),
    )(rows, queries, bias, heldk, heldv)


def turned(x, shift):
    size = lax.axis_size("tp")
    return lax.ppermute(x, "tp", [((i + shift) % size, i) for i in range(size)])


def shares(x):
    size = lax.axis_size("tp")
    me = lax.axis_index("tp")
    return [(x if s == 0 else turned(x, s), (me + s) % size) for s in range(size)]


def project(parts, weight):
    depth = parts[0][0].shape[1]
    total = None
    for block, owner in parts:
        rows = lax.dynamic_slice_in_dim(weight, owner * depth, depth, axis=0)
        term = jnp.dot(block, rows, preferred_element_type=jnp.float32)
        total = term if total is None else total + term
    return total.astype(jnp.bfloat16)


def local(tokens, query_weight, key_weight, value_weight, out_weight, chosen):
    tok_rows = tokens.shape[0]
    own_blocks = tok_rows // BLK
    key_devices = lax.axis_size("kv")
    plane = math.gcd(key_devices, PLANE)
    layers = key_devices // plane
    device = lax.axis_index("kv")
    my_layer, my_seat = device // plane, device % plane

    wanted = chosen.reshape(-1)
    holder = wanted // own_blocks
    within = wanted % own_blocks
    remote = holder != device
    slot_index = jnp.arange(wanted.shape[0])
    earlier = (
        (slot_index[None, :] < slot_index[:, None])
        & (holder[None, :] == holder[:, None])
        & remote[None, :]
    )
    places = jnp.minimum(jnp.sum(earlier.astype(jnp.int32), axis=1), CAP - 1)
    back = my_layer - holder // plane
    across = (holder % plane) ^ my_seat
    hop = (back * plane + across) * CAP + places
    asked = jnp.arange(layers * plane * CAP)
    request = jnp.sum(
        jnp.where((hop[None, :] == asked[:, None]) & remote[None, :], within[None, :], 0), axis=1
    ).reshape(layers, plane, CAP)
    ask = jnp.zeros((plane - 1, 8, 128), jnp.int32).at[:, 0, :layers * CAP].set(
        jnp.transpose(request[:, 1:], (1, 0, 2)).reshape(plane - 1, layers * CAP)
    )

    parts = shares(tokens)
    keys = project(parts, key_weight)
    values = project(parts, value_weight)
    queries = project(parts, query_weight)
    heldk, heldv = exchange(keys, values, ask, plane, layers)

    near_rows = back * own_blocks + within
    far_rows = layers * own_blocks + (back * (plane - 1) + across - 1) * CAP + places
    rows = jnp.where(across == 0, near_rows, far_rows).astype(jnp.int32)
    order = jnp.arange(TOPB)
    repeats = jnp.any(
        (chosen[:, :, None] == chosen[:, None, :]) & (order[None, None, :] < order[None, :, None]), axis=2
    )
    bias = jnp.repeat(jnp.where(repeats, -jnp.inf, 0.0).astype(jnp.float32), BLK, axis=1)
    heads_out = attend(rows, queries, bias[:, None, :], heldk, heldv)
    return project(shares(heads_out), out_weight)


def solution(mesh):
    return jax.shard_map(
        local,
        mesh=mesh,
        in_specs=(
            P("kv", "tp"),
            P(None, "tp"),
            P(None, "tp"),
            P(None, "tp"),
            P(None, "tp"),
            P("kv", None),
        ),
        out_specs=P("kv", "tp"),
        check_vma=False,
    )
```

```python
import functools
import math

import jax
import jax.numpy as jnp
from jax import lax
from jax.experimental import pallas as pl
from jax.experimental.pallas import tpu as pltpu
from jax.sharding import PartitionSpec as P

HD = 128
BLK = 64
TOPB = 16
CAP = 2
PLANE = 4
VMEM = pltpu.MemorySpace.VMEM
SMEM = pltpu.MemorySpace.SMEM


def exchange_kernel(plane, layers, shares_count, rows_ref, k_ref, v_ref, ask_ref, bias_ref, weight_any, *refs):
    parts_any = refs[:shares_count]
    (out_ref, heldk, heldv, stage, asked, asked_s, weight, parts, q_ref, picked, soft, totals,
     up_send, up_recv, side_send, side_recv, ask_send, ask_recv, move_sem, weight_sem, part_sem) = refs[shares_count:]
    own_blocks = k_ref.shape[0]
    key_heads = k_ref.shape[2] // HD
    group = out_ref.shape[1] // k_ref.shape[2]
    depth = parts_any[0].shape[1]
    fetches = [pltpu.make_async_copy(weight_any, weight, weight_sem)] + [
        pltpu.make_async_copy(part, parts.at[s], part_sem.at[s]) for s, part in enumerate(parts_any)
    ]
    for fetch in fetches:
        fetch.start()
    me = lax.axis_index("kv")
    core = lax.axis_index("tp")
    layer = me // plane
    seat = me % plane
    own = (k_ref, v_ref)
    held = (heldk, heldv)
    peers = [layer * plane + (seat ^ m) for m in range(1, plane)]
    above = layer + 1 < layers
    below = layer > 0

    def at(device):
        return {"device_id": (device, core), "device_id_type": pl.DeviceIdType.MESH}

    barrier = pltpu.get_barrier_semaphore()
    for peer in peers:
        pl.semaphore_signal(barrier, inc=1, **at(peer))

    @pl.when(above)
    def _():
        pl.semaphore_signal(barrier, inc=1, **at(me + plane))

    @pl.when(below)
    def _():
        pl.semaphore_signal(barrier, inc=1, **at(me - plane))

    between = above & below

    @pl.when(between)
    def _():
        pl.semaphore_wait(barrier, plane + 1)

    @pl.when(jnp.logical_not(between))
    def _():
        pl.semaphore_wait(barrier, plane - 1 + min(layers - 1, 1))

    def climb(k, half):
        source = own[half] if k == 0 else held[half].at[k * own_blocks:(k + 1) * own_blocks]
        return pltpu.make_async_remote_copy(
            src_ref=source,
            dst_ref=held[half].at[(k + 1) * own_blocks:(k + 2) * own_blocks],
            send_sem=up_send.at[k, half],
            recv_sem=up_recv.at[k, half],
            **at(me + plane),
        )

    def side(k, half, m):
        first = layers * own_blocks + (k * (plane - 1) + m) * CAP
        return pltpu.make_async_remote_copy(
            src_ref=stage.at[k, half, m],
            dst_ref=held[half].at[first:first + CAP],
            send_sem=side_send.at[k, half, m],
            recv_sem=side_recv.at[k, half, m],
            **at(peers[m]),
        )

    def tell(m):
        return pltpu.make_async_remote_copy(
            src_ref=ask_ref.at[m], dst_ref=asked.at[m], send_sem=ask_send.at[m], recv_sem=ask_recv.at[m],
            **at(peers[m]),
        )

    for half in range(2):
        @pl.when(above)
        def _():
            climb(0, half).start()
    for m in range(plane - 1):
        tell(m).start()
    for half in range(2):
        held[half][0:own_blocks] = own[half][...]
    for m in range(plane - 1):
        tell(m).wait()
    move = pltpu.make_async_copy(asked, asked_s, move_sem)
    move.start()
    move.wait()

    def project_queries():
        for fetch in fetches:
            fetch.wait()
        tile = min(256, weight.shape[1])
        for first in range(0, weight.shape[1], tile):
            total = None
            for share in range(shares_count):
                owner = lax.rem(core + share, shares_count)
                term = jnp.dot(
                    parts[share],
                    weight[pl.ds(pl.multiple_of(owner * depth, depth), depth), first:first + tile],
                    preferred_element_type=jnp.float32,
                )
                total = term if total is None else total + term
            q_ref[:, first:first + tile] = total.astype(jnp.bfloat16)

    for k in range(layers):
        for half in range(2):
            @pl.when(layer >= k)
            def _():
                if k > 0:
                    climb(k - 1, half).wait_recv()
                    if k + 1 < layers:
                        @pl.when(above)
                        def _():
                            climb(k, half).start()
                for m in range(plane - 1):
                    for place in range(CAP):
                        block = asked_s[m, 0, k * CAP + place]
                        taken = held[half][k * own_blocks]
                        for other in range(1, own_blocks):
                            taken = jnp.where(block == other, held[half][k * own_blocks + other], taken)
                        stage[k, half, m, place] = taken
                    side(k, half, m).start()

        if k == 0:
            project_queries()

    def drain(half):
        for k in range(layers):
            @pl.when(layer >= k)
            def _():
                for m in range(plane - 1):
                    side(k, half, m).wait()
            if k + 1 < layers:
                @pl.when(above & (layer >= k))
                def _():
                    climb(k, half).wait_send()

    def gather(source, b):
        for slot in range(TOPB):
            picked[slot * BLK:(slot + 1) * BLK, :] = source[rows_ref[b * TOPB + slot]]

    tall = group * BLK
    wide = (tall, TOPB * BLK)
    row_at = lax.broadcasted_iota(jnp.int32, wide, 0) % BLK
    col_at = lax.broadcasted_iota(jnp.int32, wide, 1)
    later = (col_at < BLK) & (col_at > row_at)

    def weigh(b, _):
        gather(heldk, b)
        first = pl.multiple_of(b * BLK, BLK)
        bias = bias_ref[b]
        for head in range(key_heads):
            q = jnp.concatenate(
                [q_ref[pl.ds(first, BLK), (head * group + g) * HD:(head * group + g + 1) * HD] for g in range(group)],
                axis=0,
            )
            scores = lax.dot_general(
                q, picked[:, head * HD:(head + 1) * HD], (((1,), (1,)), ((), ())),
                preferred_element_type=jnp.float32,
            ) * HD ** (-0.5)
            scores = jnp.where(later, -jnp.inf, scores + bias)
            peak = jnp.max(scores, axis=1, keepdims=True)
            weights = jnp.exp(scores - peak)
            total = jnp.sum(weights, axis=1, keepdims=True)
            soft[b * key_heads + head] = weights.astype(jnp.bfloat16)
            totals[b * key_heads + head] = jnp.broadcast_to(total, (tall, HD))
        return 0

    def mix(b, _):
        gather(heldv, b)
        first = pl.multiple_of(b * BLK, BLK)
        for head in range(key_heads):
            mixed = jnp.dot(
                soft[b * key_heads + head], picked[:, head * HD:(head + 1) * HD], preferred_element_type=jnp.float32
            ) / totals[b * key_heads + head]
            mixed = mixed.astype(jnp.bfloat16)
            for g in range(group):
                to = (head * group + g) * HD
                out_ref[pl.ds(first, BLK), to:to + HD] = mixed[g * BLK:(g + 1) * BLK]
        return 0

    drain(0)
    lax.fori_loop(0, own_blocks, weigh, 0)
    drain(1)
    lax.fori_loop(0, own_blocks, mix, 0)


def exchange(rows, keys, values, ask, bias, parts, query_weight, plane, layers):
    tok_rows, cols = keys.shape
    own_blocks = tok_rows // BLK
    held_blocks = layers * (own_blocks + (plane - 1) * CAP)
    width, query_cols = query_weight.shape
    tall = query_cols // cols * BLK
    steps = tok_rows // BLK * (cols // HD)
    shares_count = len(parts)
    peers = plane - 1
    dma = pltpu.SemaphoreType.DMA
    return pl.pallas_call(
        functools.partial(exchange_kernel, plane, layers, shares_count),
        out_shape=jax.ShapeDtypeStruct((tok_rows, query_cols), keys.dtype),
        in_specs=[pl.BlockSpec(memory_space=SMEM)] + [pl.BlockSpec(memory_space=VMEM)] * 4
        + [pl.BlockSpec(memory_space=pl.ANY)] * (1 + shares_count),
        out_specs=pl.BlockSpec(memory_space=VMEM),
        scratch_shapes=[
            pltpu.VMEM((held_blocks, BLK, cols), keys.dtype),
            pltpu.VMEM((held_blocks, BLK, cols), keys.dtype),
            pltpu.VMEM((layers, 2, peers, CAP, BLK, cols), keys.dtype),
            pltpu.VMEM(ask.shape, ask.dtype),
            pltpu.SMEM(ask.shape, ask.dtype),
            pltpu.VMEM((width, query_cols), keys.dtype),
            pltpu.VMEM((shares_count,) + parts[0].shape, keys.dtype),
            pltpu.VMEM((tok_rows, query_cols), keys.dtype),
            pltpu.VMEM((TOPB * BLK, cols), keys.dtype),
            pltpu.VMEM((steps, tall, TOPB * BLK), keys.dtype),
            pltpu.VMEM((steps, tall, HD), jnp.float32),
            dma((layers, 2)), dma((layers, 2)),
            dma((layers, 2, peers)), dma((layers, 2, peers)),
            dma((peers,)), dma((peers,)), dma(()), dma(()), dma((shares_count,)),
        ],
        compiler_params=pltpu.CompilerParams(
            collective_id=0, has_side_effects=True, vmem_limit_bytes=48 * 2**20
        ),
    )(
        rows, keys.reshape(own_blocks, BLK, cols), values.reshape(own_blocks, BLK, cols), ask, bias, query_weight, *parts
    )


def turned(x, shift):
    size = lax.axis_size("tp")
    return lax.ppermute(x, "tp", [((i + shift) % size, i) for i in range(size)])


def shares(x):
    size = lax.axis_size("tp")
    me = lax.axis_index("tp")
    return [(x if s == 0 else turned(x, s), (me + s) % size) for s in range(size)]


def project(parts, weight):
    depth = parts[0][0].shape[1]
    total = None
    for block, owner in parts:
        rows = lax.dynamic_slice_in_dim(weight, owner * depth, depth, axis=0)
        term = jnp.dot(block, rows, preferred_element_type=jnp.float32)
        total = term if total is None else total + term
    return total.astype(jnp.bfloat16)


def local(tokens, query_weight, key_weight, value_weight, out_weight, chosen):
    tok_rows = tokens.shape[0]
    own_blocks = tok_rows // BLK
    key_devices = lax.axis_size("kv")
    plane = math.gcd(key_devices, PLANE)
    layers = key_devices // plane
    device = lax.axis_index("kv")
    my_layer, my_seat = device // plane, device % plane

    wanted = chosen.reshape(-1)
    holder = wanted // own_blocks
    within = wanted % own_blocks
    remote = holder != device
    slot_index = jnp.arange(wanted.shape[0])
    earlier = (
        (slot_index[None, :] < slot_index[:, None])
        & (holder[None, :] == holder[:, None])
        & remote[None, :]
    )
    places = jnp.minimum(jnp.sum(earlier.astype(jnp.int32), axis=1), CAP - 1)
    back = my_layer - holder // plane
    across = (holder % plane) ^ my_seat
    hop = (back * plane + across) * CAP + places
    asked = jnp.arange(layers * plane * CAP)
    request = jnp.sum(
        jnp.where((hop[None, :] == asked[:, None]) & remote[None, :], within[None, :], 0), axis=1
    ).reshape(layers, plane, CAP)
    ask = jnp.zeros((plane - 1, 8, 128), jnp.int32).at[:, 0, :layers * CAP].set(
        jnp.transpose(request[:, 1:], (1, 0, 2)).reshape(plane - 1, layers * CAP)
    )

    parts = shares(tokens)
    keys = project(parts, key_weight)
    values = project(parts, value_weight)
    near_rows = back * own_blocks + within
    far_rows = layers * own_blocks + (back * (plane - 1) + across - 1) * CAP + places
    rows = jnp.where(across == 0, near_rows, far_rows).astype(jnp.int32)
    order = jnp.arange(TOPB)
    repeats = jnp.any(
        (chosen[:, :, None] == chosen[:, None, :]) & (order[None, None, :] < order[None, :, None]), axis=2
    )
    bias = jnp.repeat(jnp.where(repeats, -jnp.inf, 0.0).astype(jnp.float32), BLK, axis=1)
    heads_out = exchange(
        rows, keys, values, ask, bias[:, None, :], [block for block, _ in parts], query_weight, plane, layers
    )
    return project(shares(heads_out), out_weight)


def solution(mesh):
    return jax.shard_map(
        local,
        mesh=mesh,
        in_specs=(
            P("kv", "tp"),
            P(None, "tp"),
            P(None, "tp"),
            P(None, "tp"),
            P(None, "tp"),
            P("kv", None),
        ),
        out_specs=P("kv", "tp"),
        check_vma=False,
    )
```

```python
import functools
import math

import jax
import jax.numpy as jnp
from jax import lax
from jax.experimental import pallas as pl
from jax.experimental.pallas import tpu as pltpu
from jax.sharding import PartitionSpec as P

HD = 128
BLK = 64
TOPB = 16
CAP = 2
PLANE = 4
VMEM = pltpu.MemorySpace.VMEM
SMEM = pltpu.MemorySpace.SMEM


def exchange_kernel(plane, layers, shares_count, rows_ref, k_ref, v_ref, ask_ref, bias_ref, weight_any, *refs):
    parts_any = refs[:shares_count]
    (out_ref, heldk, heldv, stage, asked, asked_s, weight, parts, q_ref, picked, soft, totals,
     up_send, up_recv, side_send, side_recv, ask_send, ask_recv, move_sem, weight_sem, part_sem) = refs[shares_count:]
    own_blocks = k_ref.shape[0]
    key_heads = k_ref.shape[2] // HD
    group = out_ref.shape[1] // k_ref.shape[2]
    depth = parts_any[0].shape[1]
    fetches = [pltpu.make_async_copy(weight_any, weight, weight_sem)] + [
        pltpu.make_async_copy(part, parts.at[s], part_sem.at[s]) for s, part in enumerate(parts_any)
    ]
    for fetch in fetches:
        fetch.start()
    me = lax.axis_index("kv")
    core = lax.axis_index("tp")
    layer = me // plane
    seat = me % plane
    own = (k_ref, v_ref)
    held = (heldk, heldv)
    peers = [layer * plane + (seat ^ m) for m in range(1, plane)]
    above = layer + 1 < layers
    below = layer > 0

    def at(device):
        return {"device_id": (device, core), "device_id_type": pl.DeviceIdType.MESH}

    barrier = pltpu.get_barrier_semaphore()
    for peer in peers:
        pl.semaphore_signal(barrier, inc=1, **at(peer))

    @pl.when(above)
    def _():
        pl.semaphore_signal(barrier, inc=1, **at(me + plane))

    @pl.when(below)
    def _():
        pl.semaphore_signal(barrier, inc=1, **at(me - plane))

    between = above & below

    @pl.when(between)
    def _():
        pl.semaphore_wait(barrier, plane + 1)

    @pl.when(jnp.logical_not(between))
    def _():
        pl.semaphore_wait(barrier, plane - 1 + min(layers - 1, 1))

    def climb(k, half):
        source = own[half] if k == 0 else held[half].at[k * own_blocks:(k + 1) * own_blocks]
        return pltpu.make_async_remote_copy(
            src_ref=source,
            dst_ref=held[half].at[(k + 1) * own_blocks:(k + 2) * own_blocks],
            send_sem=up_send.at[k, half],
            recv_sem=up_recv.at[k, half],
            **at(me + plane),
        )

    def side(k, half, m):
        first = layers * own_blocks + (k * (plane - 1) + m) * CAP
        return pltpu.make_async_remote_copy(
            src_ref=stage.at[k, half, m],
            dst_ref=held[half].at[first:first + CAP],
            send_sem=side_send.at[k, half, m],
            recv_sem=side_recv.at[k, half, m],
            **at(peers[m]),
        )

    def tell(m):
        return pltpu.make_async_remote_copy(
            src_ref=ask_ref.at[m], dst_ref=asked.at[m], send_sem=ask_send.at[m], recv_sem=ask_recv.at[m],
            **at(peers[m]),
        )

    for half in range(2):
        @pl.when(above)
        def _():
            climb(0, half).start()
    for m in range(plane - 1):
        tell(m).start()
    for half in range(2):
        held[half][0:own_blocks] = own[half][...]
    for m in range(plane - 1):
        tell(m).wait()
    move = pltpu.make_async_copy(asked, asked_s, move_sem)
    move.start()
    move.wait()

    def project_queries():
        for fetch in fetches:
            fetch.wait()
        tile = min(256, weight.shape[1])
        for first in range(0, weight.shape[1], tile):
            total = None
            for share in range(shares_count):
                owner = lax.rem(core + share, shares_count)
                term = jnp.dot(
                    parts[share],
                    weight[pl.ds(pl.multiple_of(owner * depth, depth), depth), first:first + tile],
                    preferred_element_type=jnp.float32,
                )
                total = term if total is None else total + term
            q_ref[:, first:first + tile] = total.astype(jnp.bfloat16)

    for k in range(layers):
        for half in range(2):
            @pl.when(layer >= k)
            def _():
                if k > 0:
                    climb(k - 1, half).wait_recv()
                    if k + 1 < layers:
                        @pl.when(above)
                        def _():
                            climb(k, half).start()
                for m in range(plane - 1):
                    for place in range(CAP):
                        block = asked_s[m, 0, k * CAP + place]
                        taken = held[half][k * own_blocks]
                        for other in range(1, own_blocks):
                            taken = jnp.where(block == other, held[half][k * own_blocks + other], taken)
                        stage[k, half, m, place] = taken
                    side(k, half, m).start()

        if k == 0:
            project_queries()

    def drain(half):
        for k in range(layers):
            @pl.when(layer >= k)
            def _():
                for m in range(plane - 1):
                    side(k, half, m).wait()
            if k + 1 < layers:
                @pl.when(above & (layer >= k))
                def _():
                    climb(k, half).wait_send()

    def gather(source, b):
        for slot in range(TOPB):
            picked[slot * BLK:(slot + 1) * BLK, :] = source[rows_ref[b * TOPB + slot]]

    tall = group * BLK
    wide = (tall, TOPB * BLK)
    row_at = lax.broadcasted_iota(jnp.int32, wide, 0) % BLK
    col_at = lax.broadcasted_iota(jnp.int32, wide, 1)
    later = (col_at < BLK) & (col_at > row_at)

    def weigh(b, _):
        gather(heldk, b)
        first = pl.multiple_of(b * BLK, BLK)
        bias = bias_ref[b]
        for head in range(key_heads):
            q = jnp.concatenate(
                [q_ref[pl.ds(first, BLK), (head * group + g) * HD:(head * group + g + 1) * HD] for g in range(group)],
                axis=0,
            )
            scores = lax.dot_general(
                q, picked[:, head * HD:(head + 1) * HD], (((1,), (1,)), ((), ())),
                preferred_element_type=jnp.float32,
            ) * HD ** (-0.5)
            scores = jnp.where(later, -jnp.inf, scores + bias)
            peak = jnp.max(scores, axis=1, keepdims=True)
            weights = jnp.exp(scores - peak)
            total = jnp.sum(weights, axis=1, keepdims=True)
            soft[b * key_heads + head] = weights.astype(jnp.bfloat16)
            totals[b * key_heads + head] = jnp.broadcast_to(total, (tall, HD))
        return 0

    def mix(b, _):
        gather(heldv, b)
        first = pl.multiple_of(b * BLK, BLK)
        for head in range(key_heads):
            mixed = jnp.dot(
                soft[b * key_heads + head], picked[:, head * HD:(head + 1) * HD], preferred_element_type=jnp.float32
            ) / totals[b * key_heads + head]
            mixed = mixed.astype(jnp.bfloat16)
            for g in range(group):
                to = (head * group + g) * HD
                out_ref[pl.ds(first, BLK), to:to + HD] = mixed[g * BLK:(g + 1) * BLK]
        return 0

    drain(0)
    lax.fori_loop(0, own_blocks, weigh, 0)
    drain(1)
    lax.fori_loop(0, own_blocks, mix, 0)


def exchange(rows, keys, values, ask, bias, parts, query_weight, plane, layers):
    tok_rows, cols = keys.shape
    own_blocks = tok_rows // BLK
    held_blocks = layers * (own_blocks + (plane - 1) * CAP)
    width, query_cols = query_weight.shape
    tall = query_cols // cols * BLK
    steps = tok_rows // BLK * (cols // HD)
    shares_count = len(parts)
    peers = plane - 1
    dma = pltpu.SemaphoreType.DMA
    return pl.pallas_call(
        functools.partial(exchange_kernel, plane, layers, shares_count),
        out_shape=jax.ShapeDtypeStruct((tok_rows, query_cols), keys.dtype),
        in_specs=[pl.BlockSpec(memory_space=SMEM)] + [pl.BlockSpec(memory_space=VMEM)] * 4
        + [pl.BlockSpec(memory_space=pl.ANY)] * (1 + shares_count),
        out_specs=pl.BlockSpec(memory_space=VMEM),
        scratch_shapes=[
            pltpu.VMEM((held_blocks, BLK, cols), keys.dtype),
            pltpu.VMEM((held_blocks, BLK, cols), keys.dtype),
            pltpu.VMEM((layers, 2, peers, CAP, BLK, cols), keys.dtype),
            pltpu.VMEM(ask.shape, ask.dtype),
            pltpu.SMEM(ask.shape, ask.dtype),
            pltpu.VMEM((width, query_cols), keys.dtype),
            pltpu.VMEM((shares_count,) + parts[0].shape, keys.dtype),
            pltpu.VMEM((tok_rows, query_cols), keys.dtype),
            pltpu.VMEM((TOPB * BLK, cols), keys.dtype),
            pltpu.VMEM((steps, tall, TOPB * BLK), keys.dtype),
            pltpu.VMEM((steps, tall, HD), jnp.float32),
            dma((layers, 2)), dma((layers, 2)),
            dma((layers, 2, peers)), dma((layers, 2, peers)),
            dma((peers,)), dma((peers,)), dma(()), dma(()), dma((shares_count,)),
        ],
        compiler_params=pltpu.CompilerParams(
            collective_id=0, has_side_effects=True, vmem_limit_bytes=48 * 2**20
        ),
    )(
        rows, keys.reshape(own_blocks, BLK, cols), values.reshape(own_blocks, BLK, cols), ask, bias, query_weight, *parts
    )


def turned(x, shift):
    size = lax.axis_size("tp")
    return lax.ppermute(x, "tp", [((i + shift) % size, i) for i in range(size)])


def shares(x):
    size = lax.axis_size("tp")
    me = lax.axis_index("tp")
    return [(x if s == 0 else turned(x, s), (me + s) % size) for s in range(size)]


def project(parts, weight):
    depth = parts[0][0].shape[1]
    total = None
    for block, owner in parts:
        rows = lax.dynamic_slice_in_dim(weight, owner * depth, depth, axis=0)
        term = jnp.dot(block, rows, preferred_element_type=jnp.float32)
        total = term if total is None else total + term
    return total.astype(jnp.bfloat16)


def local(tokens, query_weight, key_weight, value_weight, out_weight, chosen):
    tok_rows = tokens.shape[0]
    own_blocks = tok_rows // BLK
    key_devices = lax.axis_size("kv")
    plane = math.gcd(key_devices, PLANE)
    layers = key_devices // plane
    device = lax.axis_index("kv")
    my_layer = lax.div(device, jnp.int32(plane))
    my_seat = device - my_layer * plane

    wanted = chosen.reshape(-1)
    holder = lax.div(wanted, jnp.int32(own_blocks))
    within = wanted - holder * own_blocks
    remote = holder != device
    slot_index = jnp.arange(wanted.shape[0])
    earlier = (
        (slot_index[None, :] < slot_index[:, None])
        & (holder[None, :] == holder[:, None])
        & remote[None, :]
    )
    places = jnp.minimum(jnp.sum(earlier.astype(jnp.int32), axis=1), CAP - 1)
    holder_layer = lax.div(holder, jnp.int32(plane))
    back = my_layer - holder_layer
    across = (holder - holder_layer * plane) ^ my_seat
    hop = (back * plane + across) * CAP + places
    asked = jnp.arange(layers * plane * CAP)
    request = jnp.sum(
        jnp.where((hop[None, :] == asked[:, None]) & remote[None, :], within[None, :], 0), axis=1
    ).reshape(layers, plane, CAP)
    ask = jnp.zeros((plane - 1, 8, 128), jnp.int32).at[:, 0, :layers * CAP].set(
        jnp.transpose(request[:, 1:], (1, 0, 2)).reshape(plane - 1, layers * CAP)
    )

    parts = shares(tokens)
    keys = project(parts, key_weight)
    values = project(parts, value_weight)
    near_rows = back * own_blocks + within
    far_rows = layers * own_blocks + (back * (plane - 1) + across - 1) * CAP + places
    rows = jnp.where(across == 0, near_rows, far_rows).astype(jnp.int32)
    order = jnp.arange(TOPB)
    repeats = jnp.any(
        (chosen[:, :, None] == chosen[:, None, :]) & (order[None, None, :] < order[None, :, None]), axis=2
    )
    bias = jnp.repeat(jnp.where(repeats, -jnp.inf, 0.0).astype(jnp.float32), BLK, axis=1)
    heads_out = exchange(
        rows, keys, values, ask, bias[:, None, :], [block for block, _ in parts], query_weight, plane, layers
    )
    (own_heads, seat), *others = shares(heads_out)
    first = seat * own_heads.shape[1]
    own_rows = lax.dynamic_slice_in_dim(out_weight, first, own_heads.shape[1], axis=0)
    result = jnp.dot(own_heads, own_rows, preferred_element_type=jnp.float32)
    for block, owner in others:
        result, block = lax.optimization_barrier((result, block))
        rows_of = lax.dynamic_slice_in_dim(out_weight, owner * block.shape[1], block.shape[1], axis=0)
        result = result + jnp.dot(block, rows_of, preferred_element_type=jnp.float32)
    return result.astype(jnp.bfloat16)


def solution(mesh):
    return jax.shard_map(
        local,
        mesh=mesh,
        in_specs=(
            P("kv", "tp"),
            P(None, "tp"),
            P(None, "tp"),
            P(None, "tp"),
            P(None, "tp"),
            P("kv", None),
        ),
        out_specs=P("kv", "tp"),
        check_vma=False,
    )
```
